32 devices in a mesh: ep: 8 (over z, x), tp: 4 (over y, core).
Axes of the slice: x: 2, y: 2, z: 4, core: 2. Of those that a mesh axis runs over, the one named last changes fastest.
Arguments:
- tokens: bfloat16 [4096, 2048], P(('ep', 'tp')), may hold values from -6 to 6
- expert_ids: int32 [4096, 4], P('ep'), may hold values from 0 to 7, all different within a row; in each aligned block of 128 rows (0 to 127, 128 to 255, ...) at most 64 rows name the same one
- gate_values: float32 [4096, 4], P('ep'), may hold values from 0.1 to 1
- norm_gain: float32 [2048], replicated, may hold values from 0.1 to 1.9
- gate_weight: bfloat16 [8, 2048, 1024], P('ep', None, 'tp'), may hold values from -0.125 to 0.125
- up_weight: bfloat16 [8, 2048, 1024], P('ep', None, 'tp'), may hold values from -0.125 to 0.125
- down_weight: bfloat16 [8, 1024, 2048], P('ep', 'tp'), may hold values from -0.1875 to 0.1875
- out_gain: float32 [2048], P('tp'), may hold values from 0.1 to 1.9
Outputs:
- mixed: bfloat16 [4096, 2048], P('ep', 'tp')
The draws below stay inside these ranges and needn't reach their ends.
Inputs may be any that keep to these rules, and one draw needn't show every extreme that they name: `expert_ids`: each row names 4 different experts of 0 to 7; within the rows of one device (aligned blocks of 128 rows) no expert is named more than 64 times, and in some blocks one expert is named exactly 64 times.
All inputs are finite; a program needn't handle non-finite values.
Results may differ from the reference program's by a relative error of at most 0.0025.
Values may be sent and summed in bfloat16 or wider, within the bound.
A program may use at most 64 MiB of HBM per device.

```python
import math
import jax
import jax.numpy as jnp
import numpy as np
from jax import lax

D = 2048
FF = 1024
TOP = 4
TOK_DEV = 128
CAP = 64
EXPERTS = 8
TOKENS = 4096
N_EP = 8
N_TP = 4


def level_of(rng, extent, split, least, largest):
    factor_of = 1.0
    for dim, parts in split:
        heights = jax.random.uniform(jax.random.fold_in(jax.random.fold_in(rng, 6), dim), (parts,), jnp.float32, least / len(split), largest / len(split))
        factor_of = factor_of * jnp.repeat(jnp.exp(heights), extent[dim] // parts).reshape((-1,) + (1,) * (len(extent) - 1 - dim))
    return factor_of


def routed_block(own_key, own, number, rows, count, top, limit, lean):
    order = jax.random.permutation(own_key, count)
    heavy_load, usual = load_shares(count, rows * top, limit, lean, True), load_shares(count, rows * top, limit, lean, False)
    places = jnp.arange(count)

    def named(tallies, rotation):
        used = int((tallies > 0).sum())
        fixed = max(1, used // 4)
        shifted = fixed + (places - fixed + rotation * (used - fixed)) % max(1, count - fixed)
        return jnp.zeros((count,), jnp.int32).at[order[jnp.where(places < fixed, places, shifted)]].set(jnp.asarray(tallies, jnp.int32))

    tallies = jnp.where(number % 4 == 0, named(heavy_load, number // 4), named(usual, number - number // 4 - 1))
    mixed = jax.random.permutation(jax.random.fold_in(own, 3), count)
    source_of, sink = mixed[0:count // 2 * 2:2], mixed[1:count // 2 * 2:2]
    slack = jnp.minimum(tallies[source_of] - 1, limit - tallies[sink]) // 2
    slack = jnp.where((source_of == order[0]) | (sink == order[0]) | (tallies[sink] == 0), 0, jnp.maximum(slack, 0))
    shifted = jax.random.randint(jax.random.fold_in(own, 4), (count // 2,), 0, 1 << 20) % (slack + 1)
    tallies = tallies.at[source_of].add(-shifted).at[sink].add(shifted)
    items = jnp.searchsorted(jnp.cumsum(tallies), jnp.arange(rows * top), side="right").astype(jnp.int32)
    table = items.reshape(top, rows).T
    table = table[jax.random.permutation(jax.random.fold_in(own, 1), rows)]
    rotation = jax.random.randint(jax.random.fold_in(own, 2), (rows, 1), 0, top)
    return jnp.take_along_axis(table, (jnp.arange(top)[None, :] + rotation) % top, axis=1)


def load_shares(number_of, total, limit, lean, full):
    portions = [(1 << 20) // math.isqrt(standing ** lean) + 1 for standing in range(1, number_of + 1)]
    largest = limit if full else min(limit, max(-(-total // number_of), total * portions[0] // sum(portions)))
    least = 1 if total - largest >= number_of - 1 else 0
    given, surplus = [largest] + [least] * (number_of - 1), total - largest - least * (number_of - 1)
    while surplus > 0:
        candidates = [i for i in range(1, number_of) if given[i] < largest] or [i for i in range(1, number_of) if given[i] < limit]
        mass, left = sum([portions[i] for i in candidates]), surplus
        for i in candidates:
            addition = min(limit - given[i], max(1, left * portions[i] // mass), surplus)
            given[i] = given[i] + addition
            surplus = surplus - addition
    return np.array(given)


def centred(key, dims, width, bound, pieces=(), held_as=jnp.bfloat16):
    values = width * jax.random.normal(key, dims, jnp.float32)
    if pieces:
        values = values * level_of(key, dims, pieces, -0.22, 0.18)
    return jnp.clip(values, -bound, bound).astype(held_as)


def setup_inputs(seed: int = 0) -> dict:
    key_of = jax.random.split(jax.random.key(seed), 9)
    tokens = centred(key_of[0], (TOKENS, D), 1.0, 6.0, ((0, 32),))
    expert_ids_keys = jax.random.split(jax.random.fold_in(key_of[1], 1), TOKENS // TOK_DEV)
    expert_ids_turns = jax.random.permutation(jax.random.fold_in(key_of[1], 3), TOKENS // TOK_DEV)
    expert_ids = jax.vmap(lambda own, number: routed_block(jax.random.fold_in(key_of[1], 2), own, number, TOK_DEV, EXPERTS, TOP, CAP, 2))(expert_ids_keys, expert_ids_turns).reshape((TOKENS, TOP))
    gate_values = jnp.clip(0.1 + 0.9 * jax.random.uniform(key_of[2], (TOKENS, TOP), jnp.float32) ** level_of(key_of[2], (TOKENS, TOP), ((0, 8),), -0.2, 0.2), 0.1, 1.0)
    norm_gain = jnp.clip(1.0 + 0.18 * jax.random.normal(key_of[3], (D,), jnp.float32), 0.1, 1.9)
    gate_weight = centred(key_of[4], (EXPERTS, D, FF), D ** -0.5, 0.125, ((0, 8), (2, 4)))
    up_weight = centred(key_of[5], (EXPERTS, D, FF), D ** -0.5, 0.125, ((0, 8), (2, 4)))
    down_weight = centred(key_of[6], (EXPERTS, FF, D), FF ** -0.5, 0.1875, ((0, 8), (1, 4)))
    out_gain = jnp.clip(1.0 + 0.18 * jax.random.normal(key_of[7], (D,), jnp.float32), 0.1, 1.9)
    return dict(tokens=tokens, expert_ids=expert_ids, gate_values=gate_values, norm_gain=norm_gain, gate_weight=gate_weight, up_weight=up_weight, down_weight=down_weight, out_gain=out_gain)


epsilon = 1e-05
clamp_limit = 7.0
sigmoid_alpha = 1.702

def rms_rows(values, gain):
    mean_sq = lax.optimization_barrier(jnp.mean(values * values, axis=-1, keepdims=True))
    return values * lax.rsqrt(mean_sq + epsilon) * gain

def clamped_unit(gate_part, up_part):
    glu_part = jnp.minimum(gate_part, clamp_limit)
    lin_part = jnp.clip(up_part, -clamp_limit, clamp_limit)
    return glu_part * jax.nn.sigmoid(sigmoid_alpha * glu_part) * (lin_part + 1.0)

def reference(tokens, expert_ids, gate_values, norm_gain, gate_weight, up_weight, down_weight, out_gain):
    normed = rms_rows(tokens.astype(jnp.float32), norm_gain).astype(jnp.bfloat16)
    blocks = expert_ids.reshape(N_EP * N_TP, TOK_DEV * TOP)
    onehot = (blocks[:, :, None] == jnp.arange(EXPERTS, dtype=jnp.int32)[None, None, :]).astype(jnp.int32)
    slot_num = lax.optimization_barrier(jnp.sum((jnp.cumsum(onehot, axis=1) - onehot) * onehot, axis=2)).reshape(TOKENS, TOP)
    source = (jnp.arange(TOKENS, dtype=jnp.int32) // TOK_DEV)[:, None]
    position = (source * CAP + slot_num).astype(jnp.int32)
    table_rows = N_EP * N_TP * CAP
    token_index = jnp.broadcast_to(jnp.arange(TOKENS, dtype=jnp.int32)[:, None], (TOKENS, TOP)).reshape(-1)
    padded = jnp.concatenate([normed, jnp.zeros((1, D), jnp.bfloat16)], axis=0)

    def one_expert(running, inputs):
        expert, w_gate, w_up, w_down = inputs
        chosen = expert_ids == expert
        where_row = jnp.where(chosen, position, table_rows).astype(jnp.int32)
        owner_row = jnp.full((table_rows + 1,), TOKENS, jnp.int32).at[where_row.reshape(-1)].set(token_index)
        rows_in = padded[owner_row[:table_rows]].astype(jnp.float32)
        gate_part = jnp.dot(rows_in, w_gate.astype(jnp.float32), precision=lax.Precision.HIGHEST)
        up_part = jnp.dot(rows_in, w_up.astype(jnp.float32), precision=lax.Precision.HIGHEST)
        activated = clamped_unit(gate_part, up_part).astype(jnp.bfloat16)
        activated = lax.optimization_barrier(activated).astype(jnp.float32)
        outputs = jnp.dot(activated, w_down.astype(jnp.float32), precision=lax.Precision.HIGHEST).astype(jnp.bfloat16)
        outputs = lax.optimization_barrier(outputs).astype(jnp.float32)
        outputs = jnp.concatenate([outputs, jnp.zeros((1, D), jnp.float32)], axis=0)
        for choice_k in range(TOP):
            weight = jnp.where(chosen[:, choice_k], gate_values[:, choice_k], jnp.float32(0.0))
            running = running + weight[:, None] * outputs[where_row[:, choice_k]]
        return (running, None)
    combined, _ = lax.scan(one_expert, jnp.zeros((TOKENS, D), jnp.float32), (jnp.arange(EXPERTS, dtype=jnp.int32), gate_weight, up_weight, down_weight))
    mean_sq = lax.optimization_barrier(jnp.mean(combined * combined, axis=1, keepdims=True))
    return (combined * lax.rsqrt(mean_sq + epsilon) * out_gain).astype(jnp.bfloat16)
```

```python
import functools

import jax
import jax.numpy as jnp
from jax import lax
from jax.experimental import pallas as pl
from jax.experimental.pallas import tpu as pltpu
from jax.sharding import PartitionSpec as P

epsilon = 1e-05
clamp_limit = 7.0
sigmoid_alpha = 1.702
F32 = jnp.float32
BF16 = jnp.bfloat16
MESH = pl.DeviceIdType.MESH


def clamped_unit(gate_part, up_part):
    glu_part = jnp.minimum(gate_part, clamp_limit)
    lin_part = jnp.clip(up_part, -clamp_limit, clamp_limit)
    return glu_part * jax.nn.sigmoid(sigmoid_alpha * glu_part) * (lin_part + 1.0)


def kernel(
    n_ep, n_tp,
    tokens_ref, ids_ref, values_ref, gain_ref, gate_hbm, up_hbm, down_hbm, out_gain_ref,
    mixed_ref,
    gate_all, up_all, down_all, gain_all, normed, pick, outgoing, arrived, acts, results,
    returned, combined, final,
    local_sem, gain_send, gain_recv, w_send, w_fwd, w_recv,
    d_send, d_recv, r_send, r_recv, f_send, f_recv,
):
    me = lax.axis_index("ep")
    rank = lax.axis_index("tp")
    core = lax.rem(rank, 2)
    side = lax.div(rank, 2)
    sides = n_tp // 2
    sibling = rank + 1 - 2 * core
    toks, width = tokens_ref.shape
    top = ids_ref.shape[1]
    cap = toks // 2
    part = gate_all.shape[2]
    slice_w = width // n_tp
    rows = n_ep * cap
    chunks = 2 + n_tp

    def across(d):
        return lax.rem(side + d, sides) * 2 + core

    def across_sibling(d):
        return lax.rem(side + d, sides) * 2 + 1 - core

    def ep_peer(d):
        return lax.rem(me + d, n_ep)

    def tp_peer(d):
        return lax.rem(rank + d, n_tp)

    own_copies = [
        pltpu.make_async_copy(gate_hbm.at[0], gate_all.at[rank], local_sem.at[0]),
        pltpu.make_async_copy(up_hbm.at[0], up_all.at[rank], local_sem.at[1]),
    ]
    for q in range(n_tp):
        own_copies.append(
            pltpu.make_async_copy(
                down_hbm.at[0, :, pl.ds(q * slice_w, slice_w)],
                down_all.at[q, rank],
                local_sem.at[2 + q],
            )
        )
    for copy in own_copies:
        copy.start()

    barrier = pltpu.get_barrier_semaphore()
    for d in range(1, n_ep):
        pl.semaphore_signal(
            barrier, inc=1, device_id={"ep": ep_peer(d), "tp": rank}, device_id_type=MESH
        )
    for d in range(1, n_tp):
        pl.semaphore_signal(
            barrier, inc=1, device_id={"ep": me, "tp": tp_peer(d)}, device_id_type=MESH
        )
    pl.semaphore_wait(barrier, n_ep - 1 + n_tp - 1)

    def piece(chunk, slot):
        if chunk == 0:
            return gate_all.at[slot]
        if chunk == 1:
            return up_all.at[slot]
        return down_all.at[chunk - 2, slot]

    def weight_copy(chunk, slot, sem, to):
        return pltpu.make_async_remote_copy(
            src_ref=piece(chunk, slot), dst_ref=piece(chunk, slot),
            send_sem=sem, recv_sem=w_recv.at[chunk, slot],
            device_id={"ep": me, "tp": to}, device_id_type=MESH,
        )

    sends = []
    for chunk in range(chunks):
        own_copies[chunk].wait()
        for d in range(1, sides):
            sends.append(weight_copy(chunk, rank, w_send.at[chunk, d], across(d)))
            sends[-1].start()
        sends.append(weight_copy(chunk, rank, w_send.at[chunk, 0], sibling))
        sends[-1].start()

    gain_all[rank] = out_gain_ref[...]

    step = 16

    def norm_rows(i, carry):
        at = pl.ds(pl.multiple_of(i * step, step), step)
        x = tokens_ref[at, :].astype(F32)
        mean_sq = jnp.mean(x * x, axis=-1, keepdims=True)
        normed[at, :] = (x * lax.rsqrt(mean_sq + epsilon) * gain_ref[...]).astype(BF16)
        return carry

    lax.fori_loop(0, toks // step, norm_rows, 0)

    block = pl.ds(pl.multiple_of(rank * toks, toks), toks)
    ids = ids_ref[block, :]
    values = values_ref[block, :]
    lane = lax.broadcasted_iota(jnp.int32, (toks, 128), 1)
    named = [ids[:, k:k + 1] == lane for k in range(top)]
    member = sum(jnp.where(m, 1.0, 0.0) for m in named).astype(BF16)
    row_i = lax.broadcasted_iota(jnp.int32, (toks, toks), 0)
    col_i = lax.broadcasted_iota(jnp.int32, (toks, toks), 1)
    lower = jnp.where(col_i < row_i, 1.0, 0.0).astype(BF16)
    earlier = jnp.dot(lower, member, preferred_element_type=F32)
    entry = lax.broadcasted_iota(jnp.int32, (toks, rows), 1).astype(F32)
    onehot = jnp.zeros((toks, rows), F32)
    weight = jnp.zeros((toks, rows), F32)
    for k in range(top):
        slot = jnp.sum(jnp.where(named[k], earlier, 0.0), axis=1, keepdims=True)
        target = ids[:, k:k + 1].astype(F32) * cap + slot
        hit = entry == target
        onehot = onehot + jnp.where(hit, 1.0, 0.0)
        weight = weight + jnp.where(hit, values[:, k:k + 1], 0.0)
    pick[...] = jnp.transpose(onehot).astype(BF16)

    def dispatch_rows(e, carry):
        at = pl.ds(pl.multiple_of(e * cap, cap), cap)
        for n in range(width // 512):
            outgoing[e, :, n * 512:(n + 1) * 512] = jnp.dot(
                pick[at, :], normed[:, n * 512:(n + 1) * 512], preferred_element_type=F32
            ).astype(BF16)
        return carry

    lax.fori_loop(0, n_ep, dispatch_rows, 0)
    arrived[me] = outgoing[me]

    def dispatch_copy(d):
        return pltpu.make_async_remote_copy(
            src_ref=outgoing.at[ep_peer(d)], dst_ref=arrived.at[me],
            send_sem=d_send.at[d], recv_sem=d_recv.at[me],
            device_id={"ep": ep_peer(d), "tp": rank}, device_id_type=MESH,
        )

    for d in range(1, n_ep):
        sends.append(dispatch_copy(d))
        sends[-1].start()

    def gain_copy(d):
        return pltpu.make_async_remote_copy(
            src_ref=gain_all.at[rank], dst_ref=gain_all.at[rank],
            send_sem=gain_send.at[d], recv_sem=gain_recv.at[rank],
            device_id={"ep": me, "tp": tp_peer(d)}, device_id_type=MESH,
        )

    for d in range(1, n_tp):
        sends.append(gain_copy(d))
        sends[-1].start()

    def got(ref, sem):
        pltpu.make_async_copy(ref, ref, sem).wait()

    def relay(chunk):
        for d in range(1, sides):
            slot = across(d)
            got(piece(chunk, slot), w_recv.at[chunk, slot])
            sends.append(weight_copy(chunk, slot, w_fwd.at[chunk, d], sibling))
            sends[-1].start()

    tile_e = 2

    def hidden(slot):
        def tile(i, carry):
            at = pl.ds(i * tile_e, tile_e)
            x = arrived[at].reshape(tile_e * cap, width)
            g = jnp.dot(x, gate_all[slot], preferred_element_type=F32)
            u = jnp.dot(x, up_all[slot], preferred_element_type=F32)
            acts[slot, pl.ds(pl.multiple_of(i * tile_e * cap, tile_e * cap), tile_e * cap), :] = (
                clamped_unit(g, u).astype(BF16)
            )
            return carry

        lax.fori_loop(0, n_ep // tile_e, tile, 0)

    relay(0)
    for d in range(1, n_ep):
        src = ep_peer(d)
        got(arrived.at[src], d_recv.at[src])
    hidden(rank)
    for chunk in range(2):
        got(piece(chunk, sibling), w_recv.at[chunk, sibling])
    hidden(sibling)
    relay(1)
    for d in range(1, sides):
        hidden(across(d))
    for d in range(1, sides):
        slot = across_sibling(d)
        for chunk in range(2):
            got(piece(chunk, slot), w_recv.at[chunk, slot])
        hidden(slot)

    def return_copy(q, d):
        return pltpu.make_async_remote_copy(
            src_ref=results.at[q, ep_peer(d)], dst_ref=returned.at[q, me],
            send_sem=r_send.at[q, d], recv_sem=r_recv.at[q, me],
            device_id={"ep": ep_peer(d), "tp": rank}, device_id_type=MESH,
        )

    for q in range(n_tp):
        relay(2 + q)
        got(piece(2 + q, sibling), w_recv.at[2 + q, sibling])
        for d in range(1, sides):
            slot = across_sibling(d)
            got(piece(2 + q, slot), w_recv.at[2 + q, slot])

        def tile(i, carry):
            at = pl.ds(pl.multiple_of(i * tile_e * cap, tile_e * cap), tile_e * cap)
            total = jnp.zeros((tile_e * cap, slice_w), F32)
            for s in range(n_tp):
                total = total + jnp.dot(acts[s, at, :], down_all[q, s], preferred_element_type=F32)
            results[q, pl.ds(i * tile_e, tile_e)] = total.astype(BF16).reshape(tile_e, cap, slice_w)
            return carry

        lax.fori_loop(0, n_ep // tile_e, tile, 0)
        for d in range(1, n_ep):
            sends.append(return_copy(q, d))
            sends[-1].start()
        returned[q, me] = results[q, me]

    high = weight.astype(BF16)
    rest = weight - high.astype(F32)
    mid = rest.astype(BF16)
    low = (rest - mid.astype(F32)).astype(BF16)
    total_sq = jnp.zeros((toks, 1), F32)
    for q in range(n_tp):
        for d in range(1, n_ep):
            src = ep_peer(d)
            got(returned.at[q, src], r_recv.at[q, src])
        values_in = returned[q].reshape(rows, slice_w)
        both = jnp.dot(low, values_in, preferred_element_type=F32)
        both = both + jnp.dot(mid, values_in, preferred_element_type=F32)
        both = both + jnp.dot(high, values_in, preferred_element_type=F32)
        combined[q] = both
        total_sq = total_sq + jnp.sum(both * both, axis=1, keepdims=True)
    row_scale = lax.rsqrt(total_sq / width + epsilon)
    for d in range(1, n_tp):
        src = tp_peer(d)
        got(gain_all.at[src], gain_recv.at[src])
    for q in range(n_tp):
        final[q] = (combined[q] * row_scale * gain_all[q]).astype(BF16)

    def final_copy(d):
        return pltpu.make_async_remote_copy(
            src_ref=final.at[tp_peer(d)], dst_ref=mixed_ref.at[block, :],
            send_sem=f_send.at[d], recv_sem=f_recv.at[rank],
            device_id={"ep": me, "tp": tp_peer(d)}, device_id_type=MESH,
        )

    for d in range(1, n_tp):
        sends.append(final_copy(d))
        sends[-1].start()
    mixed_ref[block, :] = final[rank]
    for d in range(1, n_tp):
        src = tp_peer(d)
        there = mixed_ref.at[pl.ds(pl.multiple_of(src * toks, toks), toks), :]
        got(there, f_recv.at[src])
    for copy in sends:
        copy.wait_send()


def local(
    tokens, expert_ids, gate_values, norm_gain, gate_weight, up_weight, down_weight, out_gain
):
    n_ep = lax.axis_size("ep")
    n_tp = lax.axis_size("tp")
    toks, width = tokens.shape
    cap = toks // 2
    rows = n_ep * cap
    part = gate_weight.shape[2]
    slice_w = width // n_tp
    chunks = 2 + n_tp
    sides = n_tp // 2
    vmem = pl.BlockSpec(memory_space=pltpu.VMEM)
    hbm = pl.BlockSpec(memory_space=pl.ANY)
    dma = pltpu.SemaphoreType.DMA
    return pl.pallas_call(
        functools.partial(kernel, n_ep, n_tp),
        out_shape=jax.ShapeDtypeStruct((n_tp * toks, slice_w), BF16),
        in_specs=[vmem, vmem, vmem, vmem, hbm, hbm, hbm, vmem],
        out_specs=vmem,
        scratch_shapes=[
            pltpu.VMEM((n_tp, width, part), BF16),
            pltpu.VMEM((n_tp, width, part), BF16),
            pltpu.VMEM((n_tp, n_tp, part, slice_w), BF16),
            pltpu.VMEM((n_tp, 1, slice_w), F32),
            pltpu.VMEM((toks, width), BF16),
            pltpu.VMEM((rows, toks), BF16),
            pltpu.VMEM((n_ep, cap, width), BF16),
            pltpu.VMEM((n_ep, cap, width), BF16),
            pltpu.VMEM((n_tp, rows, part), BF16),
            pltpu.VMEM((n_tp, n_ep, cap, slice_w), BF16),
            pltpu.VMEM((n_tp, n_ep, cap, slice_w), BF16),
            pltpu.VMEM((n_tp, toks, slice_w), F32),
            pltpu.VMEM((n_tp, toks, slice_w), BF16),
            dma((chunks,)),
            dma((n_tp,)),
            dma((n_tp,)),
            dma((chunks, sides)),
            dma((chunks, sides)),
            dma((chunks, n_tp)),
            dma((n_ep,)),
            dma((n_ep,)),
            dma((n_tp, n_ep)),
            dma((n_tp, n_ep)),
            dma((n_tp,)),
            dma((n_tp,)),
        ],
        compiler_params=pltpu.CompilerParams(
            collective_id=0, has_side_effects=True, vmem_limit_bytes=60 * 1024 * 1024
        ),
    )(
        tokens, expert_ids, gate_values, norm_gain.reshape(1, width),
        gate_weight, up_weight, down_weight, out_gain.reshape(1, slice_w),
    )


def solution(mesh):
    in_specs = (
        P(("ep", "tp"), None),
        P("ep", None),
        P("ep", None),
        P(),
        P("ep", None, "tp"),
        P("ep", None, "tp"),
        P("ep", "tp", None),
        P("tp"),
    )
    out_specs = P("ep", "tp")
    return jax.shard_map(local, mesh=mesh, in_specs=in_specs, out_specs=out_specs, check_vma=False)
```

```python
import functools

import jax
import jax.numpy as jnp
from jax import lax
from jax.experimental import pallas as pl
from jax.experimental.pallas import tpu as pltpu
from jax.sharding import PartitionSpec as P

epsilon = 1e-05
clamp_limit = 7.0
sigmoid_alpha = 1.702
F32 = jnp.float32
BF16 = jnp.bfloat16
MESH = pl.DeviceIdType.MESH


def clamped_unit(gate_part, up_part):
    glu_part = jnp.minimum(gate_part, clamp_limit)
    lin_part = jnp.clip(up_part, -clamp_limit, clamp_limit)
    return glu_part * jax.nn.sigmoid(sigmoid_alpha * glu_part) * (lin_part + 1.0)


def kernel(
    n_ep, n_tp,
    tokens_ref, ids_ref, values_ref, gain_ref, gate_hbm, up_hbm, down_hbm, out_gain_ref,
    mixed_ref,
    gate_all, up_all, down_all, gain_all, normed, pick, outgoing, arrived, acts, results,
    returned, combined, final,
    local_sem, gain_send, gain_recv, w_send, w_fwd, w_recv,
    d_send, d_recv, r_send, r_recv, f_send, f_recv,
):
    me = lax.axis_index("ep")
    rank = lax.axis_index("tp")
    core = lax.rem(rank, 2)
    side = lax.div(rank, 2)
    sides = n_tp // 2
    sibling = rank + 1 - 2 * core
    toks, width = tokens_ref.shape
    top = ids_ref.shape[0]
    cap = toks // 2
    part = gate_all.shape[2]
    slice_w = width // n_tp
    rows = n_ep * cap
    chunks = 2 + n_tp

    def across(d):
        return lax.rem(side + d, sides) * 2 + core

    def across_sibling(d):
        return lax.rem(side + d, sides) * 2 + 1 - core

    far_first = sorted(range(1, n_ep), key=lambda d: (abs(2 * d - n_ep), d))

    def ep_source(d):
        return lax.rem(me + n_ep - d, n_ep)

    def ep_peer(d):
        return lax.rem(me + d, n_ep)

    def tp_peer(d):
        return lax.rem(rank + d, n_tp)

    own_copies = [
        pltpu.make_async_copy(gate_hbm.at[0], gate_all.at[rank], local_sem.at[0]),
        pltpu.make_async_copy(up_hbm.at[0], up_all.at[rank], local_sem.at[1]),
    ]
    for q in range(n_tp):
        own_copies.append(
            pltpu.make_async_copy(
                down_hbm.at[0, :, pl.ds(q * slice_w, slice_w)],
                down_all.at[q, rank],
                local_sem.at[2 + q],
            )
        )
    for copy in own_copies:
        copy.start()

    barrier = pltpu.get_barrier_semaphore()
    for d in range(1, n_ep):
        pl.semaphore_signal(
            barrier, inc=1, device_id={"ep": ep_peer(d), "tp": rank}, device_id_type=MESH
        )
    for d in range(1, n_tp):
        pl.semaphore_signal(
            barrier, inc=1, device_id={"ep": me, "tp": tp_peer(d)}, device_id_type=MESH
        )
    pl.semaphore_wait(barrier, n_ep - 1 + n_tp - 1)

    def piece(chunk, slot):
        if chunk == 0:
            return gate_all.at[slot]
        if chunk == 1:
            return up_all.at[slot]
        return down_all.at[chunk - 2, slot]

    def weight_copy(chunk, slot, sem, to):
        return pltpu.make_async_remote_copy(
            src_ref=piece(chunk, slot), dst_ref=piece(chunk, slot),
            send_sem=sem, recv_sem=w_recv.at[chunk, slot],
            device_id={"ep": me, "tp": to}, device_id_type=MESH,
        )

    sends = []
    for chunk in range(chunks):
        own_copies[chunk].wait()
        for d in range(1, sides):
            sends.append(weight_copy(chunk, rank, w_send.at[chunk, d], across(d)))
            sends[-1].start()
        sends.append(weight_copy(chunk, rank, w_send.at[chunk, 0], sibling))
        sends[-1].start()

    gain_all[rank] = out_gain_ref[...]

    step = 16

    def norm_rows(i, carry):
        at = pl.ds(pl.multiple_of(i * step, step), step)
        x = tokens_ref[at, :].astype(F32)
        mean_sq = jnp.mean(x * x, axis=-1, keepdims=True)
        normed[at, :] = (x * lax.rsqrt(mean_sq + epsilon) * gain_ref[...]).astype(BF16)
        return carry

    lax.fori_loop(0, toks // step, norm_rows, 0)

    block = pl.ds(pl.multiple_of(rank * toks, toks), toks)
    both_t = jnp.concatenate([ids_ref[:, block].astype(F32), values_ref[:, block]], axis=0)
    both = jnp.transpose(both_t)
    ids = both[:, :top]
    values = both[:, top:]
    lane = lax.broadcasted_iota(jnp.int32, (toks, 128), 1).astype(F32)
    named = [ids[:, k:k + 1] == lane for k in range(top)]
    member = sum(jnp.where(m, 1.0, 0.0) for m in named).astype(BF16)
    row_i = lax.broadcasted_iota(jnp.int32, (toks, toks), 0)
    col_i = lax.broadcasted_iota(jnp.int32, (toks, toks), 1)
    lower = jnp.where(col_i < row_i, 1.0, 0.0).astype(BF16)
    earlier = jnp.dot(lower, member, preferred_element_type=F32)
    entry = lax.broadcasted_iota(jnp.int32, (toks, rows), 1).astype(F32)
    onehot = jnp.zeros((toks, rows), F32)
    weight = jnp.zeros((toks, rows), F32)
    for k in range(top):
        slot = jnp.sum(jnp.where(named[k], earlier, 0.0), axis=1, keepdims=True)
        target = ids[:, k:k + 1] * cap + slot
        hit = entry == target
        onehot = onehot + jnp.where(hit, 1.0, 0.0)
        weight = weight + jnp.where(hit, values[:, k:k + 1], 0.0)
    pick[...] = jnp.transpose(onehot).astype(BF16)

    def dispatch_rows(e, carry):
        at = pl.ds(pl.multiple_of(e * cap, cap), cap)
        for n in range(width // 512):
            outgoing[e, :, n * 512:(n + 1) * 512] = jnp.dot(
                pick[at, :], normed[:, n * 512:(n + 1) * 512], preferred_element_type=F32
            ).astype(BF16)
        return carry

    lax.fori_loop(0, n_ep, dispatch_rows, 0)
    arrived[me] = outgoing[me]

    def dispatch_copy(d):
        return pltpu.make_async_remote_copy(
            src_ref=outgoing.at[ep_peer(d)], dst_ref=arrived.at[me],
            send_sem=d_send.at[d], recv_sem=d_recv.at[me],
            device_id={"ep": ep_peer(d), "tp": rank}, device_id_type=MESH,
        )

    for d in far_first:
        sends.append(dispatch_copy(d))
        sends[-1].start()

    def gain_copy(d):
        return pltpu.make_async_remote_copy(
            src_ref=gain_all.at[rank], dst_ref=gain_all.at[rank],
            send_sem=gain_send.at[d], recv_sem=gain_recv.at[rank],
            device_id={"ep": me, "tp": tp_peer(d)}, device_id_type=MESH,
        )

    for d in range(1, n_tp):
        sends.append(gain_copy(d))
        sends[-1].start()

    def got(ref, sem):
        pltpu.make_async_copy(ref, ref, sem).wait()

    def relay(chunk):
        for d in range(1, sides):
            slot = across(d)
            got(piece(chunk, slot), w_recv.at[chunk, slot])
            sends.append(weight_copy(chunk, slot, w_fwd.at[chunk, d], sibling))
            sends[-1].start()

    tile_e = 2

    def hidden(slot):
        def tile(i, carry):
            at = pl.ds(i * tile_e, tile_e)
            x = arrived[at].reshape(tile_e * cap, width)
            g = jnp.dot(x, gate_all[slot], preferred_element_type=F32)
            u = jnp.dot(x, up_all[slot], preferred_element_type=F32)
            acts[slot, pl.ds(pl.multiple_of(i * tile_e * cap, tile_e * cap), tile_e * cap), :] = (
                clamped_unit(g, u).astype(BF16)
            )
            return carry

        lax.fori_loop(0, n_ep // tile_e, tile, 0)

    def hidden_block(slots, src):
        x = arrived[src]
        for slot in slots:
            g = jnp.dot(x, gate_all[slot], preferred_element_type=F32)
            u = jnp.dot(x, up_all[slot], preferred_element_type=F32)
            acts[slot, pl.ds(pl.multiple_of(src * cap, cap), cap), :] = (
                clamped_unit(g, u).astype(BF16)
            )

    for chunk in range(2):
        got(piece(chunk, sibling), w_recv.at[chunk, sibling])
    hidden_block([rank, sibling], me)
    for i, d in enumerate(far_first):
        if i == n_ep // 2 - 1:
            relay(0)
        if i == n_ep - 2:
            relay(1)
        src = ep_source(d)
        got(arrived.at[src], d_recv.at[src])
        hidden_block([rank, sibling], src)
    for d in range(1, sides):
        hidden(across(d))
    relay(2)
    for d in range(1, sides):
        slot = across_sibling(d)
        for chunk in range(2):
            got(piece(chunk, slot), w_recv.at[chunk, slot])
        hidden(slot)

    def return_copy(q, d):
        return pltpu.make_async_remote_copy(
            src_ref=results.at[q, ep_peer(d)], dst_ref=returned.at[q, me],
            send_sem=r_send.at[q, d], recv_sem=r_recv.at[q, me],
            device_id={"ep": ep_peer(d), "tp": rank}, device_id_type=MESH,
        )

    for q in range(n_tp):
        if q > 0:
            relay(2 + q)
        got(piece(2 + q, sibling), w_recv.at[2 + q, sibling])
        for d in range(1, sides):
            slot = across_sibling(d)
            got(piece(2 + q, slot), w_recv.at[2 + q, slot])

        def tile(i, carry):
            at = pl.ds(pl.multiple_of(i * tile_e * cap, tile_e * cap), tile_e * cap)
            total = jnp.zeros((tile_e * cap, slice_w), F32)
            for s in range(n_tp):
                total = total + jnp.dot(acts[s, at, :], down_all[q, s], preferred_element_type=F32)
            results[q, pl.ds(i * tile_e, tile_e)] = total.astype(BF16).reshape(tile_e, cap, slice_w)
            return carry

        lax.fori_loop(0, n_ep // tile_e, tile, 0)
        for d in far_first:
            sends.append(return_copy(q, d))
            sends[-1].start()
        returned[q, me] = results[q, me]

    high = weight.astype(BF16)
    rest = weight - high.astype(F32)
    mid = rest.astype(BF16)
    low = (rest - mid.astype(F32)).astype(BF16)
    total_sq = jnp.zeros((toks, 1), F32)
    for q in range(n_tp):
        for d in range(1, n_ep):
            src = ep_peer(d)
            got(returned.at[q, src], r_recv.at[q, src])
        values_in = returned[q].reshape(rows, slice_w)
        both = jnp.dot(low, values_in, preferred_element_type=F32)
        both = both + jnp.dot(mid, values_in, preferred_element_type=F32)
        both = both + jnp.dot(high, values_in, preferred_element_type=F32)
        combined[q] = both
        total_sq = total_sq + jnp.sum(both * both, axis=1, keepdims=True)
    row_scale = lax.rsqrt(total_sq / width + epsilon)
    for d in range(1, n_tp):
        src = tp_peer(d)
        got(gain_all.at[src], gain_recv.at[src])
    for q in range(n_tp):
        final[q] = (combined[q] * row_scale * gain_all[q]).astype(BF16)

    def final_copy(d):
        return pltpu.make_async_remote_copy(
            src_ref=final.at[tp_peer(d)], dst_ref=mixed_ref.at[block, :],
            send_sem=f_send.at[d], recv_sem=f_recv.at[rank],
            device_id={"ep": me, "tp": tp_peer(d)}, device_id_type=MESH,
        )

    for d in range(1, n_tp):
        sends.append(final_copy(d))
        sends[-1].start()
    mixed_ref[block, :] = final[rank]
    for d in range(1, n_tp):
        src = tp_peer(d)
        there = mixed_ref.at[pl.ds(pl.multiple_of(src * toks, toks), toks), :]
        got(there, f_recv.at[src])
    for copy in sends:
        copy.wait_send()


def local(
    tokens, expert_ids, gate_values, norm_gain, gate_weight, up_weight, down_weight, out_gain
):
    n_ep = lax.axis_size("ep")
    n_tp = lax.axis_size("tp")
    toks, width = tokens.shape
    cap = toks // 2
    rows = n_ep * cap
    part = gate_weight.shape[2]
    slice_w = width // n_tp
    chunks = 2 + n_tp
    sides = n_tp // 2
    vmem = pl.BlockSpec(memory_space=pltpu.VMEM)
    hbm = pl.BlockSpec(memory_space=pl.ANY)
    dma = pltpu.SemaphoreType.DMA
    return pl.pallas_call(
        functools.partial(kernel, n_ep, n_tp),
        out_shape=jax.ShapeDtypeStruct((n_tp * toks, slice_w), BF16),
        in_specs=[vmem, vmem, vmem, vmem, hbm, hbm, hbm, vmem],
        out_specs=vmem,
        scratch_shapes=[
            pltpu.VMEM((n_tp, width, part), BF16),
            pltpu.VMEM((n_tp, width, part), BF16),
            pltpu.VMEM((n_tp, n_tp, part, slice_w), BF16),
            pltpu.VMEM((n_tp, 1, slice_w), F32),
            pltpu.VMEM((toks, width), BF16),
            pltpu.VMEM((rows, toks), BF16),
            pltpu.VMEM((n_ep, cap, width), BF16),
            pltpu.VMEM((n_ep, cap, width), BF16),
            pltpu.VMEM((n_tp, rows, part), BF16),
            pltpu.VMEM((n_tp, n_ep, cap, slice_w), BF16),
            pltpu.VMEM((n_tp, n_ep, cap, slice_w), BF16),
            pltpu.VMEM((n_tp, toks, slice_w), F32),
            pltpu.VMEM((n_tp, toks, slice_w), BF16),
            dma((chunks,)),
            dma((n_tp,)),
            dma((n_tp,)),
            dma((chunks, sides)),
            dma((chunks, sides)),
            dma((chunks, n_tp)),
            dma((n_ep,)),
            dma((n_ep,)),
            dma((n_tp, n_ep)),
            dma((n_tp, n_ep)),
            dma((n_tp,)),
            dma((n_tp,)),
        ],
        compiler_params=pltpu.CompilerParams(
            collective_id=0, has_side_effects=True, vmem_limit_bytes=60 * 1024 * 1024
        ),
    )(
        tokens, expert_ids.T, gate_values.T, norm_gain.reshape(1, width),
        gate_weight, up_weight, down_weight, out_gain.reshape(1, slice_w),
    )


def solution(mesh):
    in_specs = (
        P(("ep", "tp"), None),
        P("ep", None),
        P("ep", None),
        P(),
        P("ep", None, "tp"),
        P("ep", None, "tp"),
        P("ep", "tp", None),
        P("tp"),
    )
    out_specs = P("ep", "tp")
    return jax.shard_map(local, mesh=mesh, in_specs=in_specs, out_specs=out_specs, check_vma=False)
```

```python
import functools

import jax
import jax.numpy as jnp
from jax import lax
from jax.experimental import pallas as pl
from jax.experimental.pallas import tpu as pltpu
from jax.sharding import PartitionSpec as P

epsilon = 1e-05
clamp_limit = 7.0
sigmoid_alpha = 1.702
F32 = jnp.float32
BF16 = jnp.bfloat16
MESH = pl.DeviceIdType.MESH


def clamped_unit(gate_part, up_part):
    glu_part = jnp.minimum(gate_part, clamp_limit)
    lin_part = jnp.clip(up_part, -clamp_limit, clamp_limit)
    return glu_part * jax.nn.sigmoid(sigmoid_alpha * glu_part) * (lin_part + 1.0)


def kernel(
    n_ep, n_tp,
    tokens_ref, ids_ref, values_ref, gain_ref, gate_hbm, up_hbm, down_hbm, out_gain_ref,
    mixed_ref,
    gate_all, up_all, down_all, gain_all, normed, pick, outgoing, arrived, acts, results,
    returned, combined, final,
    local_sem, gain_send, gain_recv, w_send, w_fwd, w_recv,
    d_send, d_recv, r_send, r_recv, f_send, f_recv,
):
    me = lax.axis_index("ep")
    rank = lax.axis_index("tp")
    core = lax.rem(rank, 2)
    side = lax.div(rank, 2)
    sides = n_tp // 2
    sibling = rank + 1 - 2 * core
    toks, width = tokens_ref.shape
    top = ids_ref.shape[0]
    cap = toks // 2
    part = gate_all.shape[2]
    slice_w = width // n_tp
    rows = n_ep * cap
    chunks = 2 + n_tp

    def across(d):
        return lax.rem(side + d, sides) * 2 + core

    def across_sibling(d):
        return lax.rem(side + d, sides) * 2 + 1 - core

    far_first = sorted(range(1, n_ep), key=lambda d: (abs(2 * d - n_ep), d))

    def ep_source(d):
        return lax.rem(me + n_ep - d, n_ep)

    def ep_peer(d):
        return lax.rem(me + d, n_ep)

    def tp_peer(d):
        return lax.rem(rank + d, n_tp)

    own_copies = [
        pltpu.make_async_copy(gate_hbm.at[0], gate_all.at[rank], local_sem.at[0]),
        pltpu.make_async_copy(up_hbm.at[0], up_all.at[rank], local_sem.at[1]),
    ]
    for q in range(n_tp):
        own_copies.append(
            pltpu.make_async_copy(
                down_hbm.at[0, :, pl.ds(q * slice_w, slice_w)],
                down_all.at[q, rank],
                local_sem.at[2 + q],
            )
        )
    for copy in own_copies:
        copy.start()

    barrier = pltpu.get_barrier_semaphore()
    for d in range(1, n_ep):
        pl.semaphore_signal(
            barrier, inc=1, device_id={"ep": ep_peer(d), "tp": rank}, device_id_type=MESH
        )
    for d in range(1, n_tp):
        pl.semaphore_signal(
            barrier, inc=1, device_id={"ep": me, "tp": tp_peer(d)}, device_id_type=MESH
        )
    pl.semaphore_wait(barrier, n_ep - 1 + n_tp - 1)

    def piece(chunk, slot):
        if chunk == 0:
            return gate_all.at[slot]
        if chunk == 1:
            return up_all.at[slot]
        return down_all.at[chunk - 2, slot]

    def weight_copy(chunk, slot, sem, to):
        return pltpu.make_async_remote_copy(
            src_ref=piece(chunk, slot), dst_ref=piece(chunk, slot),
            send_sem=sem, recv_sem=w_recv.at[chunk, slot],
            device_id={"ep": me, "tp": to}, device_id_type=MESH,
        )

    sends = []
    for chunk in range(chunks):
        own_copies[chunk].wait()
        for d in range(1, sides):
            sends.append(weight_copy(chunk, rank, w_send.at[chunk, d], across(d)))
            sends[-1].start()
        sends.append(weight_copy(chunk, rank, w_send.at[chunk, 0], sibling))
        sends[-1].start()

    gain_all[rank] = out_gain_ref[...]

    step = 16

    def norm_rows(i, carry):
        at = pl.ds(pl.multiple_of(i * step, step), step)
        x = tokens_ref[at, :].astype(F32)
        mean_sq = jnp.mean(x * x, axis=-1, keepdims=True)
        normed[at, :] = (x * lax.rsqrt(mean_sq + epsilon) * gain_ref[...]).astype(BF16)
        return carry

    lax.fori_loop(0, toks // step, norm_rows, 0)

    block = pl.ds(pl.multiple_of(rank * toks, toks), toks)
    both_t = jnp.concatenate([ids_ref[:, block].astype(F32), values_ref[:, block]], axis=0)
    both = jnp.transpose(both_t)
    ids = both[:, :top]
    values = both[:, top:]
    lane = lax.broadcasted_iota(jnp.int32, (toks, 128), 1).astype(F32)
    named = [ids[:, k:k + 1] == lane for k in range(top)]
    member = sum(jnp.where(m, 1.0, 0.0) for m in named).astype(BF16)
    row_i = lax.broadcasted_iota(jnp.int32, (toks, toks), 0)
    col_i = lax.broadcasted_iota(jnp.int32, (toks, toks), 1)
    lower = jnp.where(col_i < row_i, 1.0, 0.0).astype(BF16)
    earlier = jnp.dot(lower, member, preferred_element_type=F32)
    entry = lax.broadcasted_iota(jnp.int32, (toks, rows), 1).astype(F32)
    onehot = jnp.zeros((toks, rows), F32)
    weight = jnp.zeros((toks, rows), F32)
    for k in range(top):
        slot = jnp.sum(jnp.where(named[k], earlier, 0.0), axis=1, keepdims=True)
        target = ids[:, k:k + 1] * cap + slot
        hit = entry == target
        onehot = onehot + jnp.where(hit, 1.0, 0.0)
        weight = weight + jnp.where(hit, values[:, k:k + 1], 0.0)
    pick[...] = jnp.transpose(onehot).astype(BF16)

    def dispatch_rows(e):
        at = pl.ds(pl.multiple_of(e * cap, cap), cap)
        for n in range(width // 512):
            outgoing[e, :, n * 512:(n + 1) * 512] = jnp.dot(
                pick[at, :], normed[:, n * 512:(n + 1) * 512], preferred_element_type=F32
            ).astype(BF16)

    def dispatch_copy(d):
        return pltpu.make_async_remote_copy(
            src_ref=outgoing.at[ep_peer(d)], dst_ref=arrived.at[me],
            send_sem=d_send.at[d], recv_sem=d_recv.at[me],
            device_id={"ep": ep_peer(d), "tp": rank}, device_id_type=MESH,
        )

    for i, d in enumerate(far_first + [0]):
        dispatch_rows(ep_peer(d))
        if i > 0:
            sends.append(dispatch_copy(far_first[i - 1]))
            sends[-1].start()
    arrived[me] = outgoing[me]

    def gain_copy(d):
        return pltpu.make_async_remote_copy(
            src_ref=gain_all.at[rank], dst_ref=gain_all.at[rank],
            send_sem=gain_send.at[d], recv_sem=gain_recv.at[rank],
            device_id={"ep": me, "tp": tp_peer(d)}, device_id_type=MESH,
        )

    for d in range(1, n_tp):
        sends.append(gain_copy(d))
        sends[-1].start()

    def got(ref, sem):
        pltpu.make_async_copy(ref, ref, sem).wait()

    def relay(chunk):
        for d in range(1, sides):
            slot = across(d)
            got(piece(chunk, slot), w_recv.at[chunk, slot])
            sends.append(weight_copy(chunk, slot, w_fwd.at[chunk, d], sibling))
            sends[-1].start()

    tile_e = 2

    def hidden(slot):
        def tile(i, carry):
            at = pl.ds(i * tile_e, tile_e)
            x = arrived[at].reshape(tile_e * cap, width)
            g = jnp.dot(x, gate_all[slot], preferred_element_type=F32)
            u = jnp.dot(x, up_all[slot], preferred_element_type=F32)
            acts[slot, pl.ds(pl.multiple_of(i * tile_e * cap, tile_e * cap), tile_e * cap), :] = (
                clamped_unit(g, u).astype(BF16)
            )
            return carry

        lax.fori_loop(0, n_ep // tile_e, tile, 0)

    def hidden_block(slots, src):
        x = arrived[src]
        for slot in slots:
            g = jnp.dot(x, gate_all[slot], preferred_element_type=F32)
            u = jnp.dot(x, up_all[slot], preferred_element_type=F32)
            acts[slot, pl.ds(pl.multiple_of(src * cap, cap), cap), :] = (
                clamped_unit(g, u).astype(BF16)
            )

    for chunk in range(2):
        got(piece(chunk, sibling), w_recv.at[chunk, sibling])
    hidden_block([rank, sibling], me)
    for i, d in enumerate(far_first):
        if i == n_ep // 2 - 1:
            relay(0)
        if i == n_ep - 2:
            relay(1)
        src = ep_source(d)
        got(arrived.at[src], d_recv.at[src])
        hidden_block([rank, sibling], src)
    for d in range(1, sides):
        hidden(across(d))
    relay(2)
    for d in range(1, sides):
        slot = across_sibling(d)
        for chunk in range(2):
            got(piece(chunk, slot), w_recv.at[chunk, slot])
        hidden(slot)

    def return_copy(q, d):
        return pltpu.make_async_remote_copy(
            src_ref=results.at[q, ep_peer(d)], dst_ref=returned.at[q, me],
            send_sem=r_send.at[q, d], recv_sem=r_recv.at[q, me],
            device_id={"ep": ep_peer(d), "tp": rank}, device_id_type=MESH,
        )

    for q in range(n_tp):
        if q > 0:
            relay(2 + q)
        got(piece(2 + q, sibling), w_recv.at[2 + q, sibling])
        for d in range(1, sides):
            slot = across_sibling(d)
            got(piece(2 + q, slot), w_recv.at[2 + q, slot])

        def tile(i, carry):
            at = pl.ds(pl.multiple_of(i * tile_e * cap, tile_e * cap), tile_e * cap)
            total = jnp.zeros((tile_e * cap, slice_w), F32)
            for s in range(n_tp):
                total = total + jnp.dot(acts[s, at, :], down_all[q, s], preferred_element_type=F32)
            results[q, pl.ds(i * tile_e, tile_e)] = total.astype(BF16).reshape(tile_e, cap, slice_w)
            return carry

        lax.fori_loop(0, n_ep // tile_e, tile, 0)
        for d in far_first:
            sends.append(return_copy(q, d))
            sends[-1].start()
        returned[q, me] = results[q, me]

    high = weight.astype(BF16)
    rest = weight - high.astype(F32)
    mid = rest.astype(BF16)
    low = (rest - mid.astype(F32)).astype(BF16)
    total_sq = jnp.zeros((toks, 1), F32)
    for q in range(n_tp):
        for d in range(1, n_ep):
            src = ep_peer(d)
            got(returned.at[q, src], r_recv.at[q, src])
        values_in = returned[q].reshape(rows, slice_w)
        both = jnp.dot(low, values_in, preferred_element_type=F32)
        both = both + jnp.dot(mid, values_in, preferred_element_type=F32)
        both = both + jnp.dot(high, values_in, preferred_element_type=F32)
        combined[q] = both
        total_sq = total_sq + jnp.sum(both * both, axis=1, keepdims=True)
    row_scale = lax.rsqrt(total_sq / width + epsilon)
    for d in range(1, n_tp):
        src = tp_peer(d)
        got(gain_all.at[src], gain_recv.at[src])
    for q in range(n_tp):
        final[q] = (combined[q] * row_scale * gain_all[q]).astype(BF16)

    def final_copy(d):
        return pltpu.make_async_remote_copy(
            src_ref=final.at[tp_peer(d)], dst_ref=mixed_ref.at[block, :],
            send_sem=f_send.at[d], recv_sem=f_recv.at[rank],
            device_id={"ep": me, "tp": tp_peer(d)}, device_id_type=MESH,
        )

    for d in range(1, n_tp):
        sends.append(final_copy(d))
        sends[-1].start()
    mixed_ref[block, :] = final[rank]
    for d in range(1, n_tp):
        src = tp_peer(d)
        there = mixed_ref.at[pl.ds(pl.multiple_of(src * toks, toks), toks), :]
        got(there, f_recv.at[src])
    for copy in sends:
        copy.wait_send()


def local(
    tokens, expert_ids, gate_values, norm_gain, gate_weight, up_weight, down_weight, out_gain
):
    n_ep = lax.axis_size("ep")
    n_tp = lax.axis_size("tp")
    toks, width = tokens.shape
    cap = toks // 2
    rows = n_ep * cap
    part = gate_weight.shape[2]
    slice_w = width // n_tp
    chunks = 2 + n_tp
    sides = n_tp // 2
    vmem = pl.BlockSpec(memory_space=pltpu.VMEM)
    hbm = pl.BlockSpec(memory_space=pl.ANY)
    dma = pltpu.SemaphoreType.DMA
    return pl.pallas_call(
        functools.partial(kernel, n_ep, n_tp),
        out_shape=jax.ShapeDtypeStruct((n_tp * toks, slice_w), BF16),
        in_specs=[vmem, vmem, vmem, vmem, hbm, hbm, hbm, vmem],
        out_specs=vmem,
        scratch_shapes=[
            pltpu.VMEM((n_tp, width, part), BF16),
            pltpu.VMEM((n_tp, width, part), BF16),
            pltpu.VMEM((n_tp, n_tp, part, slice_w), BF16),
            pltpu.VMEM((n_tp, 1, slice_w), F32),
            pltpu.VMEM((toks, width), BF16),
            pltpu.VMEM((rows, toks), BF16),
            pltpu.VMEM((n_ep, cap, width), BF16),
            pltpu.VMEM((n_ep, cap, width), BF16),
            pltpu.VMEM((n_tp, rows, part), BF16),
            pltpu.VMEM((n_tp, n_ep, cap, slice_w), BF16),
            pltpu.VMEM((n_tp, n_ep, cap, slice_w), BF16),
            pltpu.VMEM((n_tp, toks, slice_w), F32),
            pltpu.VMEM((n_tp, toks, slice_w), BF16),
            dma((chunks,)),
            dma((n_tp,)),
            dma((n_tp,)),
            dma((chunks, sides)),
            dma((chunks, sides)),
            dma((chunks, n_tp)),
            dma((n_ep,)),
            dma((n_ep,)),
            dma((n_tp, n_ep)),
            dma((n_tp, n_ep)),
            dma((n_tp,)),
            dma((n_tp,)),
        ],
        compiler_params=pltpu.CompilerParams(
            collective_id=0, has_side_effects=True, vmem_limit_bytes=60 * 1024 * 1024
        ),
    )(
        tokens, expert_ids.T, gate_values.T, norm_gain.reshape(1, width),
        gate_weight, up_weight, down_weight, out_gain.reshape(1, slice_w),
    )


def solution(mesh):
    in_specs = (
        P(("ep", "tp"), None),
        P("ep", None),
        P("ep", None),
        P(),
        P("ep", None, "tp"),
        P("ep", None, "tp"),
        P("ep", "tp", None),
        P("tp"),
    )
    out_specs = P("ep", "tp")
    return jax.shard_map(local, mesh=mesh, in_specs=in_specs, out_specs=out_specs, check_vma=False)
```
